32 devices in a mesh: grp: 2 (over y), fs: 4 (over z), tp: 4 (over x, core).
Axes of the slice: x: 2, y: 2, z: 4, core: 2. Of those that a mesh axis runs over, the one named last changes fastest.
Arguments:
- tokens: bfloat16 [8, 1024, 2048], P(('grp', 'fs'), None, 'tp'), parts along dimension 0, may hold values from -6 to 6
- mix_gain: float32 [2048], replicated, may hold values from 0.1 to 1.9
- in_matrix: float32 [2048, 1024], P('fs', 'tp'), may hold values from -0.125 to 0.125
- in_scale: float32 [1, 1024], P(None, 'tp'), may hold values from 0.5 to 2
- pool_mix: bfloat16 [8, 128, 128], P('tp'), may hold values from -0.5 to 0.5
- pool_scale: float32 [1, 1024], P(None, 'tp'), may hold values from 0.1 to 1.9
- out_matrix: float32 [1024, 2048], P('tp', 'fs'), may hold values from -0.25 to 0.25
- out_scale: float32 [1, 2048], P(None, 'fs'), may hold values from 0.5 to 2
- ffn_gain: float32 [2048], replicated, may hold values from 0.1 to 1.9
- gate_matrix: float32 [2048, 5632], P('fs', 'tp'), may hold values from -0.125 to 0.125
- gate_scale: float32 [1, 5632], P(None, 'tp'), may hold values from 0.5 to 2
- up_matrix: float32 [2048, 5632], P('fs', 'tp'), may hold values from -0.125 to 0.125
- up_scale: float32 [1, 5632], P(None, 'tp'), may hold values from 0.5 to 2
- gate_taps: float32 [3, 5632], P(None, 'tp'), may hold values from -4 to 4
- up_taps: float32 [3, 5632], P(None, 'tp'), may hold values from -4 to 4
- down_matrix: float32 [5632, 2048], P('tp', 'fs'), may hold values from -0.109375 to 0.109375
- down_scale: float32 [1, 2048], P(None, 'fs'), may hold values from 0.5 to 2
Outputs:
- layer_out: bfloat16 [8, 1024, 2048], P(('grp', 'fs'), None, 'tp'), parts along dimension 0
The draws below stay inside these ranges and needn't reach their ends.
There are 2 independent parts, one for each index of `grp`. The reference program is written for one: setup_inputs(seed, part) draws one part's arguments, and reference() takes and returns one part's arrays. A program takes and returns all parts, laid end to end along the dimension named above; an argument that names none is the same for every part. Nothing has to cross between parts.
All inputs are finite; a program needn't handle non-finite values.
Results may differ from the reference program's by a relative error of at most 0.025.
Values may be sent and summed in bfloat16 or wider, within the bound.
A program may use at most 128 MiB of HBM per device.

```python
import math
import jax
import jax.numpy as jnp
from jax import lax

D = 2048
BLOCKS = 8
BLOCK_CH = 128
FF = 5632
LEN = 1024
PW = 1024
SEQS = 4
COL_GROUPS = 4


def raised(array, stream_key, source, target, shards_of, factor):
    def block_of(dim):
        return (jnp.arange(array.shape[dim]) // (array.shape[dim] // shards_of)).reshape((-1,) + (1,) * (array.ndim - 1 - dim))

    near = jax.random.permutation(stream_key, shards_of)[block_of(target)]
    far = (block_of(target) + shards_of // 2) % shards_of
    return jnp.where((block_of(source) == near) | (block_of(source) == far), factor * array, array)


def levels(stream_key, shape, pieces, least, top_value):
    level, own = 1.0, jax.random.fold_in(stream_key, 6)
    for dim, shards_of in pieces:
        steps = jnp.exp(jax.random.uniform(jax.random.fold_in(own, dim), (shards_of,), jnp.float32, least / len(pieces), top_value / len(pieces)))
        level = level * jnp.repeat(steps, shape[dim] // shards_of).reshape([-1 if axis == dim else 1 for axis in range(len(shape))])
    return level


def bell_draw(own_key, shape, deviation, reach, pieces=(), kind=jnp.bfloat16):
    drawn = deviation * jax.random.normal(own_key, shape, jnp.float32)
    if pieces:
        drawn = drawn * levels(own_key, shape, pieces, -0.22, 0.18)
    return jnp.clip(drawn, -reach, reach).astype(kind)


def gaussian_with(rng, shape, width, reach, cuts, heavy, held_as=jnp.bfloat16):
    drawn = width * jax.random.normal(rng, shape, jnp.float32)
    if cuts:
        drawn = drawn * levels(rng, shape, cuts, -0.22, 0.18)
    return jnp.clip(raised(drawn, jax.random.fold_in(rng, 3), *heavy), -reach, reach).astype(held_as)


def setup_inputs(seed: int = 0, part: int = 0) -> dict:
    streams_of = jax.random.split(jax.random.key(seed), 18)
    part_keys = jax.random.split(jax.random.fold_in(streams_of[17], part), 18)
    tokens = bell_draw(part_keys[0], (SEQS, LEN, D), 1.0, 6.0, ((0, 4), (2, 4)))
    mix_gain = jnp.clip(1.0 + 0.18 * jax.random.normal(streams_of[1], (D,), jnp.float32), 0.1, 1.9)
    in_matrix = bell_draw(streams_of[2], (D, PW), D ** -0.5, 0.125, ((0, 4), (1, 4)), jnp.float32)
    in_scale = jnp.clip(jnp.exp(math.log(2.0) - 1.3862944 * jax.random.uniform(streams_of[3], (1, PW), jnp.float32) ** levels(streams_of[3], (1, PW), ((1, 4),), -0.2, 0.2)), 0.5, 2.0)
    pool_mix = bell_draw(streams_of[4], (BLOCKS, BLOCK_CH, BLOCK_CH), BLOCK_CH ** -0.5, 0.5, ((0, 4),))
    pool_scale = jnp.clip(1.0 + 0.18 * jax.random.normal(streams_of[5], (1, PW), jnp.float32), 0.1, 1.9)
    out_matrix = gaussian_with(streams_of[6], (PW, D), PW ** -0.5, 0.25, ((0, 4), (1, 4)), (0, 1, 4, 2.0), jnp.float32)
    out_scale = jnp.clip(jnp.exp(math.log(2.0) - 1.3862944 * jax.random.uniform(streams_of[7], (1, D), jnp.float32) ** levels(streams_of[7], (1, D), ((1, 4),), -0.2, 0.2)), 0.5, 2.0)
    ffn_gain = jnp.clip(1.0 + 0.18 * jax.random.normal(streams_of[8], (D,), jnp.float32), 0.1, 1.9)
    gate_matrix = bell_draw(streams_of[9], (D, FF), D ** -0.5, 0.125, ((0, 4), (1, 4)), jnp.float32)
    gate_scale = jnp.clip(jnp.exp(math.log(2.0) - 1.3862944 * jax.random.uniform(streams_of[10], (1, FF), jnp.float32) ** levels(streams_of[10], (1, FF), ((1, 4),), -0.2, 0.2)), 0.5, 2.0)
    up_matrix = bell_draw(streams_of[11], (D, FF), D ** -0.5, 0.125, ((0, 4), (1, 4)), jnp.float32)
    up_scale = jnp.clip(jnp.exp(math.log(2.0) - 1.3862944 * jax.random.uniform(streams_of[12], (1, FF), jnp.float32) ** levels(streams_of[12], (1, FF), ((1, 4),), -0.2, 0.2)), 0.5, 2.0)
    gate_taps = bell_draw(streams_of[13], (3, FF), 0.58, 4.0, ((1, 4),), jnp.float32)
    up_taps = bell_draw(streams_of[14], (3, FF), 0.58, 4.0, ((1, 4),), jnp.float32)
    down_matrix = gaussian_with(streams_of[15], (FF, D), FF ** -0.5, 0.109375, ((0, 4), (1, 4)), (0, 1, 4, 2.0), jnp.float32)
    down_scale = jnp.clip(jnp.exp(math.log(2.0) - 1.3862944 * jax.random.uniform(streams_of[16], (1, D), jnp.float32) ** levels(streams_of[16], (1, D), ((1, 4),), -0.2, 0.2)), 0.5, 2.0)
    return {"tokens": tokens, "mix_gain": mix_gain, "in_matrix": in_matrix, "in_scale": in_scale, "pool_mix": pool_mix, "pool_scale": pool_scale, "out_matrix": out_matrix, "out_scale": out_scale, "ffn_gain": ffn_gain, "gate_matrix": gate_matrix, "gate_scale": gate_scale, "up_matrix": up_matrix, "up_scale": up_scale, "gate_taps": gate_taps, "up_taps": up_taps, "down_matrix": down_matrix, "down_scale": down_scale}


eps = 1e-06
widest_span = 16

def norm_rows(tok_rows, norm_gain):
    values = tok_rows.astype(jnp.float32)
    scaled = values * lax.rsqrt(lax.optimization_barrier(jnp.mean(values * values, axis=-1, keepdims=True)) + eps)
    return (scaled * norm_gain.astype(jnp.float32)).astype(jnp.bfloat16)

def span_widths(block_ids):
    return jnp.left_shift(jnp.ones_like(block_ids), (1 + 4 * block_ids // BLOCKS).astype(jnp.int32))

def trailing_gap(projected, windows):
    values = projected.astype(jnp.float32)
    length = values.shape[0]
    running = values
    for offset in range(1, widest_span):
        shifted = jnp.pad(values[:length - offset], ((offset, 0), (0, 0)))
        running = running + jnp.where(windows[None, :] > offset, shifted, jnp.zeros_like(shifted))
    positions = jnp.arange(length, dtype=jnp.int32)[:, None]
    counts = jnp.minimum(positions + 1, windows[None, :]).astype(jnp.float32)
    return (running / counts - values).astype(jnp.bfloat16)

def causal_taps(linear, tap_table):
    values = linear.astype(jnp.float32)
    length = values.shape[0]
    back_one = jnp.pad(values[:length - 1], ((1, 0), (0, 0)))
    back_two = jnp.pad(values[:length - 2], ((2, 0), (0, 0)))
    return tap_table[2] * values + tap_table[1] * back_one + tap_table[0] * back_two

def grouped_product(operand, matrix, scales):
    narrow = operand.shape[1] // COL_GROUPS
    cast_matrix = matrix.astype(jnp.bfloat16)
    running = jnp.zeros((operand.shape[0], matrix.shape[1]), jnp.float32)
    for member in range(COL_GROUPS):
        partial_value = jnp.dot(operand[:, member * narrow:(member + 1) * narrow], cast_matrix[member * narrow:(member + 1) * narrow], preferred_element_type=jnp.float32) * scales
        rounded = lax.optimization_barrier(partial_value.astype(jnp.bfloat16))
        running = running + rounded.astype(jnp.float32)
    return running

def reference(tokens, mix_gain, in_matrix, in_scale, pool_mix, pool_scale, out_matrix, out_scale, ffn_gain, gate_matrix, gate_scale, up_matrix, up_scale, gate_taps, up_taps, down_matrix, down_scale):
    windows = jnp.repeat(span_widths(jnp.arange(BLOCKS, dtype=jnp.int32)), BLOCK_CH)
    in_cast = in_matrix.astype(jnp.bfloat16)
    gate_cast = gate_matrix.astype(jnp.bfloat16)
    up_cast = up_matrix.astype(jnp.bfloat16)

    def single(sequence):
        normed = norm_rows(sequence, mix_gain)
        projected = (jnp.dot(normed, in_cast, preferred_element_type=jnp.float32) * in_scale).astype(jnp.bfloat16)
        spread = trailing_gap(projected, windows)
        blocks = spread.reshape(-1, BLOCKS, BLOCK_CH).astype(jnp.float32)
        block_mixed = jnp.einsum('lbc,bce->lbe', blocks, pool_mix.astype(jnp.float32)).reshape(-1, PW)
        pooled = (block_mixed * pool_scale).astype(jnp.bfloat16)
        mixing = grouped_product(pooled, out_matrix, out_scale)
        residual = (sequence.astype(jnp.float32) + mixing).astype(jnp.bfloat16)
        normed_ffn = norm_rows(residual, ffn_gain)
        gate_lin = (jnp.dot(normed_ffn, gate_cast, preferred_element_type=jnp.float32) * gate_scale).astype(jnp.bfloat16)
        up_lin = (jnp.dot(normed_ffn, up_cast, preferred_element_type=jnp.float32) * up_scale).astype(jnp.bfloat16)
        hidden = (jax.nn.silu(causal_taps(gate_lin, gate_taps)) * causal_taps(up_lin, up_taps)).astype(jnp.bfloat16)
        feed_out = grouped_product(hidden, down_matrix, down_scale)
        return (residual.astype(jnp.float32) + feed_out).astype(jnp.bfloat16)
    return lax.map(single, tokens)
```

```python
import jax
import jax.numpy as jnp
from jax import lax
from jax.sharding import PartitionSpec as P


BLOCKS = 8


eps = 1e-06
widest_span = 16


def norm_rows(tok_rows, norm_gain):
    values = tok_rows.astype(jnp.float32)
    scaled = values * lax.rsqrt(jnp.mean(values * values, axis=-1, keepdims=True) + eps)
    return (scaled * norm_gain).astype(jnp.bfloat16)


def span_widths(block_ids):
    return jnp.left_shift(jnp.ones_like(block_ids), 1 + 4 * block_ids // BLOCKS)


def trailing_gap(projected, windows):
    values = projected.astype(jnp.float32)
    length = values.shape[0]
    running = values
    for offset in range(1, widest_span):
        shifted = jnp.pad(values[: length - offset], ((offset, 0), (0, 0)))
        running = running + jnp.where(windows[None, :] > offset, shifted, jnp.zeros_like(shifted))
    positions = jnp.arange(length, dtype=jnp.int32)[:, None]
    counts = jnp.minimum(positions + 1, windows[None, :]).astype(jnp.float32)
    return (running / counts - values).astype(jnp.bfloat16)


def causal_taps(linear, tap_table):
    values = linear.astype(jnp.float32)
    length = values.shape[0]
    back_one = jnp.pad(values[: length - 1], ((1, 0), (0, 0)))
    back_two = jnp.pad(values[: length - 2], ((2, 0), (0, 0)))
    return tap_table[2] * values + tap_table[1] * back_one + tap_table[0] * back_two


def fold_rows(operand, portion):
    return jnp.dot(operand, portion, preferred_element_type=jnp.float32)


def row_halves(shard):
    rows = shard.shape[0] // 2
    mine = lax.axis_index("grp")
    first, second = shard[:rows], shard[rows:]
    return (
        jnp.where(mine == 0, first, second),
        jnp.where(mine == 0, second, first),
    )


def across_groups(value):
    return lax.ppermute(value, "grp", [(0, 1), (1, 0)])


def half_gather(half):
    return lax.all_gather(half, "fs", axis=0, tiled=False)


def others(stacked):
    count = stacked.shape[0]
    here = lax.axis_index("fs")
    return jnp.stack(
        [
            lax.dynamic_index_in_dim(stacked, lax.rem(here + k, count), 0, keepdims=False)
            for k in range(1, count)
        ]
    )


def tp_swap(value, distance):
    count = lax.axis_size("tp")
    return lax.ppermute(value, "tp", [(i, (i + distance) % count) for i in range(count)])


def core_swap(value):
    count = lax.axis_size("tp")
    return lax.ppermute(value, "tp", [(i, i ^ 1) for i in range(count)])


def tp_gather(block, also=None):
    count = lax.axis_size("tp")
    me = lax.axis_index("tp")
    chips = count // 2
    parity = lax.rem(me, 2)
    same = [block] + [tp_swap(block, 2 * j) for j in range(1, chips)]
    if also is not None:
        same, also = tied(same, also)
    crossed = [core_swap(item) for item in same]
    blocks = []
    for chip in range(chips):
        pairs = []
        for group in (same, crossed):
            picked = group[0]
            for j in range(1, chips):
                source = lax.rem(me // 2 - j + chips, chips)
                picked = jnp.where(source == chip, group[j], picked)
            pairs.append(picked)
        blocks.append(jnp.where(parity == 0, pairs[0], pairs[1]))
        blocks.append(jnp.where(parity == 0, pairs[1], pairs[0]))
    return jnp.concatenate(blocks, axis=1), also


def tied(value, other):
    return lax.optimization_barrier((value, other))


def tp_scatter_sum(blocks, also=None):
    count = len(blocks)
    me = lax.axis_index("tp")
    chips = count // 2
    even = lax.rem(me, 2) == 0
    rounded = [item.astype(jnp.bfloat16) for item in blocks]
    pair_sums = []
    for chip in range(chips):
        keep = jnp.where(even, rounded[2 * chip], rounded[2 * chip + 1])
        give = jnp.where(even, rounded[2 * chip + 1], rounded[2 * chip])
        pair_sums.append(keep.astype(jnp.float32) + core_swap(give).astype(jnp.float32))
    chip_index = me // 2

    def for_chip(target):
        picked = pair_sums[0]
        for chip in range(1, chips):
            picked = jnp.where(target == chip, pair_sums[chip], picked)
        return picked

    total = for_chip(chip_index)
    outs = [
        for_chip(lax.rem(chip_index + j, chips)).astype(jnp.bfloat16) for j in range(1, chips)
    ]
    if also is not None:
        outs, also = tied(outs, also)
    for j in range(1, chips):
        total = total + tp_swap(outs[j - 1], 2 * j).astype(jnp.float32)
    return total, also


def shards(
    tokens,
    mix_gain,
    in_matrix,
    in_scale,
    pool_mix,
    pool_scale,
    out_matrix,
    out_scale,
    ffn_gain,
    gate_matrix,
    gate_scale,
    up_matrix,
    up_scale,
    gate_taps,
    up_taps,
    down_matrix,
    down_scale,
):
    half = jnp.bfloat16
    length = tokens.shape[1]
    own_width = tokens.shape[2]
    local_rows = tokens.reshape(length, own_width)
    fs_count = lax.axis_size("fs")
    tp_count = lax.axis_size("tp")
    group = lax.axis_index("grp")
    fs_index = lax.axis_index("fs")

    in_mine, _ = row_halves(in_matrix.astype(half))
    out_mine, _ = row_halves((out_matrix * out_scale).astype(half))
    small_mine = half_gather(jnp.stack([in_mine, out_mine.reshape(in_mine.shape)]))
    small_theirs = across_groups(small_mine)
    small_first = jnp.where(group == 0, small_mine, small_theirs)
    small_second = jnp.where(group == 0, small_theirs, small_mine)
    in_full = jnp.stack([small_first[:, 0], small_second[:, 0]], axis=1).reshape(
        fs_count * in_matrix.shape[0], in_matrix.shape[1]
    )
    out_shape = (fs_count,) + out_mine.shape
    out_full = jnp.concatenate(
        [small_first[:, 1].reshape(out_shape), small_second[:, 1].reshape(out_shape)], axis=1
    )

    wide = []

    def start_wide(cast):
        mine, theirs_here = row_halves(cast)
        mine_all = half_gather(mine)
        wide.append((mine_all, theirs_here))

    start_wide(gate_matrix.astype(half))

    gathered, _ = tp_gather(local_rows)
    gathered, up_cast = tied(gathered, up_matrix.astype(half))
    start_wide(up_cast)
    normed = norm_rows(gathered, mix_gain)
    pieces = 2
    piece_width = down_matrix.shape[1] // pieces
    down_cast = (down_matrix * down_scale).astype(half)
    down_cast, normed = lax.optimization_barrier((down_cast, normed))
    downs = []
    for piece in range(pieces):
        mine, theirs_here = row_halves(
            down_cast[:, piece * piece_width : (piece + 1) * piece_width]
        )
        mine_all = half_gather(mine)
        downs.append((mine_all, theirs_here))

    width_in = in_matrix.shape[1]
    projected = (fold_rows(normed, in_full) * in_scale).astype(half)
    local_blocks = pool_mix.shape[0]
    block_width = pool_mix.shape[1]
    block_ids = lax.axis_index("tp") * local_blocks + jnp.arange(local_blocks, dtype=jnp.int32)
    windows = jnp.repeat(span_widths(block_ids), block_width)
    spread = trailing_gap(projected, windows)
    block_mixed = jnp.einsum(
        "lbc,bce->lbe",
        spread.reshape(length, local_blocks, block_width),
        pool_mix,
        preferred_element_type=jnp.float32,
    ).reshape(length, width_in)
    pooled = (block_mixed * pool_scale).astype(half)
    per_device = fs_count // tp_count
    mixing, gate_send = tp_scatter_sum(
        [
            jnp.concatenate(
                [
                    fold_rows(pooled, out_full[d * per_device + i])
                    for i in range(per_device)
                ],
                axis=1,
            )
            for d in range(tp_count)
        ],
        others(wide[0][0]),
    )
    gate_theirs = across_groups(gate_send)
    residual = (local_rows.astype(jnp.float32) + mixing).astype(half)

    gathered_ffn, up_mine = tp_gather(residual, wide[1][0])
    up_theirs = across_groups(others(up_mine))
    normed_ffn = norm_rows(gathered_ffn, ffn_gain)
    rows = gate_matrix.shape[0] // 2
    split = normed_ffn.reshape(length, fs_count, 2, rows)
    first, second = split[:, :, 0], split[:, :, 1]
    x_mine = jnp.where(group == 0, first, second).reshape(length, fs_count * rows)
    x_theirs = jnp.where(group == 0, second, first)
    x_here = lax.dynamic_index_in_dim(x_theirs, fs_index, 1, keepdims=False)
    x_others = jnp.concatenate(
        [
            lax.dynamic_index_in_dim(
                x_theirs, lax.rem(fs_index + k, fs_count), 1, keepdims=False
            )
            for k in range(1, fs_count)
        ],
        axis=1,
    )
    x_mine, x_here, x_others = lax.optimization_barrier((x_mine, x_here, x_others))
    units = gate_matrix.shape[1]

    def widen(x_parts, parts, scale):
        total = sum(fold_rows(x, w.reshape(-1, units)) for x, w in zip(x_parts, parts))
        return (total * scale).astype(half)

    x_parts = (x_mine, x_here, x_others)
    gate_lin = widen(x_parts, (wide[0][0], wide[0][1], gate_theirs), gate_scale)
    gate_lin, mine_first, x_parts = lax.optimization_barrier((gate_lin, downs[0][0], x_parts))
    theirs_first = across_groups(others(mine_first))
    up_lin = widen(x_parts, (up_mine, wide[1][1], up_theirs), up_scale)
    up_lin, mine_second = tied(up_lin, downs[1][0])
    theirs_second = across_groups(others(mine_second))
    lins = [gate_lin, up_lin]
    hidden = (
        jax.nn.silu(causal_taps(lins[0], gate_taps)) * causal_taps(lins[1], up_taps)
    ).astype(half)
    middle = units // 2
    h_first, h_second = hidden[:, :middle], hidden[:, middle:]
    h_mine = jnp.where(group == 0, h_first, h_second)
    h_theirs = jnp.where(group == 0, h_second, h_first)
    h_mine, h_theirs = lax.optimization_barrier((h_mine, h_theirs))
    results = []
    arrivals = ((mine_first, theirs_first), (mine_second, theirs_second))
    for (_, theirs_here), (mine_all, arrived) in zip(downs, arrivals):
        theirs = jnp.concatenate([theirs_here[None], arrived])
        blocks = []
        for f in range(fs_count):
            slot = lax.rem(f - fs_index + fs_count, fs_count)
            blocks.append(
                fold_rows(h_mine, mine_all[f])
                + fold_rows(
                    h_theirs, lax.dynamic_index_in_dim(theirs, slot, 0, keepdims=False)
                )
            )
        results.append(
            tp_scatter_sum(
                [
                    jnp.concatenate(blocks[d * per_device : (d + 1) * per_device], axis=1)
                    for d in range(tp_count)
                ],
            )[0]
        )
    feed_out = jnp.stack(
        [item.reshape(length, per_device, piece_width) for item in results], axis=2
    ).reshape(length, own_width)
    result = (residual.astype(jnp.float32) + feed_out).astype(half)
    return result.reshape(1, length, result.shape[1])


def solution(mesh):
    return jax.shard_map(
        shards,
        mesh=mesh,
        in_specs=(
            P(("grp", "fs"), None, "tp"),
            P(),
            P("fs", "tp"),
            P(None, "tp"),
            P("tp", None, None),
            P(None, "tp"),
            P("tp", "fs"),
            P(None, "fs"),
            P(),
            P("fs", "tp"),
            P(None, "tp"),
            P("fs", "tp"),
            P(None, "tp"),
            P(None, "tp"),
            P(None, "tp"),
            P("tp", "fs"),
            P(None, "fs"),
        ),
        out_specs=P(("grp", "fs"), None, "tp"),
        check_vma=False,
    )
```
